32 devices in a mesh: sp: 16 (over z, y, x), tp: 2 (over core).
Axes of the slice: x: 2, y: 2, z: 4, core: 2. Of those that a mesh axis runs over, the one named last changes fastest.
Arguments:
- tokens: bfloat16 [6144, 2048], P(('sp', 'tp')), may hold values from -6 to 6
- query_weight: bfloat16 [2048, 1024], P(None, 'tp'), may hold values from -0.125 to 0.125
- key_weight: bfloat16 [2048, 1024], P(None, 'tp'), may hold values from -0.125 to 0.125
- value_weight: bfloat16 [2048, 1024], P(None, 'tp'), may hold values from -0.125 to 0.125
- query_gain: float32 [64], replicated, may hold values from 0.5 to 16
- key_gain: float32 [64], replicated, may hold values from 0.5 to 16
- log_gate_total: float32 [6144, 16], P('sp', 'tp'), may hold values from -877 to 0, as said below
- output_weight: bfloat16 [1024, 2048], P('tp'), may hold values from -0.1875 to 0.1875
Outputs:
- mixed: bfloat16 [6144, 2048], P(('sp', 'tp'))
The draws below stay inside these ranges and needn't reach their ends.
Inputs may be any that keep to these rules, and one draw needn't show every extreme that they name: `log_gate_total`: each column never rises from one position to the next.
All inputs are finite; a program needn't handle non-finite values.
Results may differ from the reference program's by a relative error of at most 0.014.
The reference program's roundings to bfloat16 on the way count: a program that leaves them out, or rounds other values in their place, can miss the bound.
Values may be sent and summed in bfloat16 or wider, within the bound.
A program may use at most 128 MiB of HBM per device.

```python
import math
import jax
import jax.numpy as jnp
from jax import lax

D = 2048
HEADS = 16
HEAD_SIZE = 64
TOK_DEV = 384
TOKENS = 6144
N_TP = 2


def gain_draw(key, salt_number):
    values = jax.random.uniform(jax.random.fold_in(key, salt_number), (HEAD_SIZE,), jnp.float32, 0.5, 1.5)
    return values


def draw_query_gain(key, part):
    return gain_draw(key, 21)


def draw_key_gain(key, part):
    return gain_draw(key, 22)


def draw_log_gate_total(key, part):
    head_order = jax.random.permutation(jax.random.fold_in(key, 31), HEADS)
    slow_count = HEADS // 2
    is_slow = head_order < slow_count
    slow_rate = jax.random.uniform(jax.random.fold_in(key, 32), (HEADS,), jnp.float32, 0.3, 1.5) / TOKENS
    fast_rate = 1.0 / jax.random.uniform(jax.random.fold_in(key, 33), (HEADS,), jnp.float32, 30.0, 100.0)
    base_rate = jnp.where(is_slow, slow_rate, fast_rate)
    block_factor = jnp.exp(jax.random.uniform(jax.random.fold_in(key, 34), (TOKENS // TOK_DEV, HEADS), jnp.float32, -0.8, 0.8))
    block_factor = jnp.repeat(block_factor, TOK_DEV, axis=0)
    jitter = jax.random.uniform(jax.random.fold_in(key, 35), (TOKENS, HEADS), jnp.float32, 0.2, 1.8)
    steps_down = -base_rate[None, :] * block_factor * jitter
    return jnp.cumsum(steps_down, axis=0)


def levels(key, dims, cuts, least, top_value):
    def one(dim, parts):
        heights = jax.random.uniform(jax.random.fold_in(jax.random.fold_in(key, 6), dim), (parts,), jnp.float32, least / len(cuts), top_value / len(cuts))
        return jnp.repeat(jnp.exp(heights), dims[dim] // parts).reshape((-1,) + (1,) * (len(dims) - dim - 1))

    factor_of = one(*cuts[0])
    for cut in cuts[1:]:
        factor_of = factor_of * one(*cut)
    return factor_of


def normal_values(own_key, extent, deviation, most, cuts=(), kind=jnp.bfloat16):
    drawn = jax.random.normal(own_key, extent, jnp.float32) * deviation
    if len(cuts) > 0:
        drawn = levels(own_key, extent, cuts, -0.22, 0.18) * drawn
    return jnp.clip(drawn, min=-most, max=most).astype(kind)


def setup_inputs(seed: int = 0) -> dict:
    key_of = jax.random.split(jax.random.key(seed), 9)
    return {
        "tokens": normal_values(key_of[0], (TOKENS, D), 1.0, 6.0, ((0, 32),)),
        "query_weight": normal_values(key_of[1], (D, HEADS * HEAD_SIZE), D ** -0.5, 0.125, ((1, 2),)),
        "key_weight": normal_values(key_of[2], (D, HEADS * HEAD_SIZE), D ** -0.5, 0.125, ((1, 2),)),
        "value_weight": normal_values(key_of[3], (D, HEADS * HEAD_SIZE), D ** -0.5, 0.125, ((1, 2),)),
        "query_gain": draw_query_gain(jax.random.fold_in(key_of[8], 71), 0),
        "key_gain": draw_key_gain(jax.random.fold_in(key_of[8], 71), 0),
        "log_gate_total": draw_log_gate_total(jax.random.fold_in(key_of[8], 71), 0),
        "output_weight": normal_values(key_of[7], (HEADS * HEAD_SIZE, D), (HEADS * HEAD_SIZE) ** -0.5, 0.1875, ((0, 2),)),
    }


NORM_EPS = 1e-06

def head_norm(raw, gain, head_count):
    row_count = raw.shape[0]
    split = raw.reshape(row_count, head_count, -1)
    scaled = split * lax.rsqrt(lax.optimization_barrier(jnp.mean(split * split, axis=-1, keepdims=True)) + NORM_EPS) * gain.astype(jnp.float32)
    return scaled.reshape(row_count, -1).astype(jnp.bfloat16)

def reference(tokens, query_weight, key_weight, value_weight, query_gain, key_gain, log_gate_total, output_weight):
    queries = head_norm(jnp.dot(tokens, query_weight, preferred_element_type=jnp.float32), query_gain, HEADS)
    keys = head_norm(jnp.dot(tokens, key_weight, preferred_element_type=jnp.float32), key_gain, HEADS)
    values = jnp.dot(tokens, value_weight, preferred_element_type=jnp.float32).astype(jnp.bfloat16)
    seq_len = tokens.shape[0]
    block_rows = math.gcd(seq_len, 512)
    key_pos = jnp.arange(seq_len, dtype=jnp.int32)
    score_scale = HEAD_SIZE ** (-0.5)

    def one_head(inputs):
        query_head, key_head, value_head, gate_head = inputs

        def one_block(block_index):
            first_row = (block_index * block_rows).astype(jnp.int32)
            query_block = lax.dynamic_slice_in_dim(query_head, first_row, block_rows, 0)
            gate_block = lax.dynamic_slice_in_dim(gate_head, first_row, block_rows, 0)
            scores = jnp.dot(query_block, key_head.T, preferred_element_type=jnp.float32) * score_scale
            scores = scores + gate_block[:, None] - gate_head[None, :]
            query_pos = first_row + jnp.arange(block_rows, dtype=jnp.int32)
            scores = jnp.where(query_pos[:, None] >= key_pos[None, :], scores, -jnp.inf)
            row_max = lax.optimization_barrier(jnp.max(scores, axis=1, keepdims=True))
            weights = jnp.exp(scores - row_max)
            totals = lax.optimization_barrier(jnp.sum(weights, axis=1, keepdims=True))
            summed = jnp.dot(weights.astype(jnp.bfloat16), value_head, preferred_element_type=jnp.float32)
            return (summed / totals).astype(jnp.bfloat16)
        blocks = lax.map(one_block, jnp.arange(seq_len // block_rows, dtype=jnp.int32))
        return blocks.reshape(seq_len, HEAD_SIZE)

    def by_heads(matrix):
        return matrix.reshape(seq_len, HEADS, HEAD_SIZE).transpose(1, 0, 2)
    attended = lax.map(one_head, (by_heads(queries), by_heads(keys), by_heads(values), log_gate_total.T))
    attended = attended.transpose(1, 0, 2).reshape(seq_len, HEADS * HEAD_SIZE)
    group_cols = HEADS * HEAD_SIZE // N_TP
    mixed = jnp.zeros((seq_len, D), jnp.float32)
    for part_index in range(N_TP):
        lower = part_index * group_cols
        partial_sum = jnp.dot(attended[:, lower:lower + group_cols], output_weight[lower:lower + group_cols], preferred_element_type=jnp.float32)
        rounded = lax.optimization_barrier(partial_sum.astype(jnp.bfloat16))
        mixed = mixed + rounded.astype(jnp.float32)
    return mixed.astype(jnp.bfloat16)
```

```python
import functools
import math

import jax
import jax.numpy as jnp
from jax import lax
from jax.experimental import pallas as pl
from jax.experimental.pallas import tpu as pltpu
from jax.sharding import PartitionSpec as P

NORM_EPS = 1e-06
LANES = 128
GATE_ROWS = 16
F32 = jnp.float32
BF16 = jnp.bfloat16
MESH = pl.DeviceIdType.MESH


def split3(value):
    first = value.astype(BF16).astype(F32)
    rest = value - first
    second = rest.astype(BF16).astype(F32)
    third = (rest - second).astype(BF16).astype(F32)
    return first, second, third


def kernel(
    n_sp, n_tp, heads, size, shard_rows, tile, block,
    tok_ref, wq_ref, wk_ref, wv_ref, qg_ref, kg_ref, gate_ref, wo_ref,
    out_ref,
    tok_all, wq, wk, wv, wo, stage, slab, kbuf, vbuf, att_stage, att_all, att_rows, part, part_in,
    w_sem, tok_send, tok_recv, slab_send, slab_recv, fwd_send, att_send, att_recv, part_send, part_recv,
):
    me = lax.axis_index("sp")
    tp = lax.axis_index("tp")
    core = lax.rem(tp, 2)
    pair = tp - core
    own_rows = tok_ref.shape[0]
    width = heads * size
    copies = n_sp // (2 * heads)
    k_row = size + GATE_ROWS
    v_row = 2 * k_row
    head_of_chip = me // copies
    src_tp = pair + head_of_chip // heads
    src_head = lax.rem(head_of_chip, heads)
    rank = lax.rem(me, copies) * 2 + core
    group = 2 * copies
    tokens_total = n_sp * shard_rows
    rounds = tokens_total // tile // group
    per_tile = tile // LANES
    per_chunk = shard_rows // LANES

    loads = [
        pltpu.make_async_copy(src, dst, w_sem.at[at])
        for at, (src, dst) in enumerate(
            ((wq_ref, wq), (wk_ref, wk), (wv_ref, wv), (wo_ref, wo), (tok_ref, tok_all.at[tp]))
        )
    ]

    def tok_copy(step):
        peer = lax.rem(tp + step, n_tp)
        return pltpu.make_async_remote_copy(
            src_ref=tok_ref, dst_ref=tok_all.at[tp],
            send_sem=tok_send.at[step], recv_sem=tok_recv.at[step],
            device_id=(me, peer), device_id_type=MESH,
        )

    tok_copies = [tok_copy(step) for step in range(1, n_tp)]
    for copy in tok_copies:
        copy.start()
    loads[4].start()
    for load in loads[:4]:
        load.start()

    row = lax.broadcasted_iota(jnp.int32, (GATE_ROWS, shard_rows), 0)
    for h in range(heads):
        a, b, c = split3(gate_ref[h : h + 1, :])
        one = jnp.ones((GATE_ROWS, shard_rows), F32)
        zero = jnp.zeros((GATE_ROWS, shard_rows), F32)
        first = jnp.where(row == 0, a, jnp.where(row == 1, b, jnp.where(row == 2, c, zero)))
        k_side = jnp.where((row >= 3) & (row < 6), one, first)
        later = jnp.where(row == 3, a, jnp.where(row == 4, b, jnp.where(row == 5, c, zero)))
        q_side = jnp.where(row < 3, -one, later)
        stage[h, size : size + GATE_ROWS, :] = q_side.astype(BF16)
        stage[h, k_row + size : k_row + size + GATE_ROWS, :] = k_side.astype(BF16)

    loads[4].wait()
    for copy in tok_copies:
        copy.wait()

    def slab_copy(h, r, source):
        chip = (core * heads + h) * copies + r
        target = pair + lax.rem(source, 2)
        return chip, target, pltpu.make_async_remote_copy(
            src_ref=stage.at[h], dst_ref=slab.at[source],
            send_sem=slab_send.at[h * copies + r], recv_sem=slab_recv.at[source],
            device_id=(chip, target), device_id_type=MESH,
        )

    def slab_local(h):
        return pltpu.make_async_copy(stage.at[h], slab.at[me], slab_recv.at[me])

    for load in loads[:3]:
        load.wait()

    cols = math.gcd(width, 256)
    group_heads = cols // size

    def project(j, carry):
        at = pl.ds(pl.multiple_of(j * cols, cols), cols)
        for base, weight, gain in ((0, wq, qg_ref), (k_row, wk, kg_ref), (v_row, wv, None)):
            raw = jnp.dot(
                tok_all[...].reshape(n_tp * own_rows, tok_all.shape[2]), weight[:, at],
                preferred_element_type=F32,
            )
            flat = raw.T
            for g in range(group_heads):
                part_t = flat[g * size : (g + 1) * size, :]
                if gain is not None:
                    mean = jnp.mean(part_t * part_t, axis=0, keepdims=True)
                    part_t = part_t * lax.rsqrt(mean + NORM_EPS) * gain[...]
                stage[j * group_heads + g, base : base + size, :] = part_t.astype(BF16)

        def send(at_send, carry):
            h = j * group_heads + at_send // copies
            r = lax.rem(at_send, copies)
            chip, target, copy = slab_copy(h, r, me)
            mine = (chip == me) & (target == tp)

            @pl.when(jnp.logical_not(mine))
            def _():
                copy.start()

            @pl.when(mine)
            def _():
                slab_local(h).start()

            return carry

        lax.fori_loop(0, group_heads * copies, send, 0)
        return carry

    lax.fori_loop(0, width // cols, project, 0)

    def fwd_copy(source):
        return pltpu.make_async_remote_copy(
            src_ref=slab.at[source], dst_ref=slab.at[source],
            send_sem=fwd_send.at[source], recv_sem=slab_recv.at[source],
            device_id=(me, pair + 1 - core), device_id_type=MESH,
        )

    def take(k, carry):
        source = 2 * k + core
        fwd_copy(source).wait_recv()
        fwd_copy(source).start()
        return carry

    lax.fori_loop(0, n_sp // 2, take, 0)

    def take_sibling(k, carry):
        fwd_copy(2 * k + 1 - core).wait_recv()
        return carry

    lax.fori_loop(0, n_sp // 2, take_sibling, 0)

    def prepare(i, carry):
        at = pl.ds(pl.multiple_of(i * shard_rows, shard_rows), shard_rows)
        kbuf[at, :] = slab[i, k_row : k_row + LANES, :].T
        vbuf[:, at] = slab[i, v_row : v_row + size, :]
        return carry

    lax.fori_loop(0, n_sp, prepare, 0)

    def att_copy(g, slot):
        owner = g // per_chunk
        where_to = lax.rem(g, per_chunk)
        return owner, pltpu.make_async_remote_copy(
            src_ref=att_stage.at[slot], dst_ref=att_all.at[src_head, where_to],
            send_sem=att_send.at[slot], recv_sem=att_recv.at[src_head * per_chunk + where_to],
            device_id=(owner, src_tp), device_id_type=MESH,
        )

    def att_local(g, slot):
        where_to = lax.rem(g, per_chunk)
        return pltpu.make_async_copy(
            att_stage.at[slot], att_all.at[src_head, where_to],
            att_recv.at[src_head * per_chunk + where_to],
        )

    def tile_of(k):
        return k * group + jnp.where(lax.rem(k, 2) == 0, rank, group - 1 - rank)

    def attend(k, carry):
        j = tile_of(k)
        pieces = []
        for p in range(per_tile):
            g = j * per_tile + p
            lane = pl.ds(pl.multiple_of(lax.rem(g, per_chunk) * LANES, LANES), LANES)
            pieces.append(slab[g // per_chunk, 0:k_row, lane])
        q = jnp.concatenate(pieces, axis=1)
        q = jnp.concatenate([q, jnp.zeros((LANES - k_row, tile), BF16)], axis=0)

        def step(i, state, masked):
            top, total, acc = state
            at = pl.ds(pl.multiple_of(i * block, block), block)
            s = jnp.dot(kbuf[at, :], q, preferred_element_type=F32)
            if masked:
                key = i * block + lax.broadcasted_iota(jnp.int32, (block, tile), 0)
                query = j * tile + lax.broadcasted_iota(jnp.int32, (block, tile), 1)
                s = jnp.where(key <= query, s, -jnp.inf)
            new_top = jnp.maximum(top, jnp.max(s, axis=0, keepdims=True))
            p = jnp.exp(s - new_top)
            scale = jnp.exp(top - new_top)
            total = total * scale + jnp.sum(p, axis=0, keepdims=True)
            acc = acc * scale + jnp.dot(vbuf[:, at], p.astype(BF16), preferred_element_type=F32)
            return new_top, total, acc

        state = (
            jnp.full((1, tile), -1e30, F32),
            jnp.zeros((1, tile), F32),
            jnp.zeros((size, tile), F32),
        )
        full = j * tile // block
        state = lax.fori_loop(0, full, lambda i, st: step(i, st, False), state)
        top, total, acc = step(full, state, True)
        done = (acc / total).astype(BF16)
        for p in range(per_tile):
            slot = k * per_tile + p
            att_stage[slot] = done[:, p * LANES : (p + 1) * LANES]
        for p in range(per_tile):
            slot = k * per_tile + p
            g = j * per_tile + p
            owner, copy = att_copy(g, slot)
            mine = (owner == me) & (src_tp == tp)

            @pl.when(jnp.logical_not(mine))
            def _():
                copy.start()

            @pl.when(mine)
            def _():
                att_local(g, slot).start()

        return carry

    lax.fori_loop(0, rounds, attend, 0)

    loads[3].wait()

    def att_wait(at, carry):
        h = at // per_chunk
        p = lax.rem(at, per_chunk)
        pltpu.make_async_remote_copy(
            src_ref=att_stage.at[0], dst_ref=att_all.at[h, p],
            send_sem=att_send.at[0], recv_sem=att_recv.at[at],
            device_id=(me, pair + 1 - core), device_id_type=MESH,
        ).wait_recv()
        return carry

    lax.fori_loop(0, heads * per_chunk, att_wait, 0)
    for p in range(per_chunk):
        joined = jnp.concatenate([att_all[h, p] for h in range(heads)], axis=0)
        att_rows[p * LANES : (p + 1) * LANES, :] = joined.T

    def part_copy(step):
        peer = lax.rem(tp + step, n_tp)
        return pltpu.make_async_remote_copy(
            src_ref=part.at[peer], dst_ref=part_in.at[step],
            send_sem=part_send.at[step], recv_sem=part_recv.at[step],
            device_id=(me, peer), device_id_type=MESH,
        )

    model = wo.shape[1]
    out_cols = math.gcd(model, 512)

    def project_rows(step, carry):
        peer = lax.rem(tp + step, n_tp)
        rows = att_rows[pl.ds(pl.multiple_of(peer * own_rows, math.gcd(own_rows, LANES)), own_rows), :]

        def columns(c, carry):
            at = pl.ds(pl.multiple_of(c * out_cols, out_cols), out_cols)
            part[peer, :, at] = jnp.dot(rows, wo[:, at], preferred_element_type=F32).astype(BF16)
            return carry

        lax.fori_loop(0, model // out_cols, columns, 0)
        return carry

    for step in range(1, n_tp):
        project_rows(step, 0)
        part_copy(step).start()
    project_rows(0, 0)
    for step in range(1, n_tp):
        part_copy(step).wait_recv()

    def finish(c, carry):
        at = pl.ds(pl.multiple_of(c * out_cols, out_cols), out_cols)
        mixed = part[tp, :, at].astype(F32)
        for step in range(1, n_tp):
            mixed = mixed + part_in[step, :, at].astype(F32)
        out_ref[:, at] = mixed.astype(BF16)
        return carry

    lax.fori_loop(0, model // out_cols, finish, 0)

    for step in range(1, n_tp):
        part_copy(step).wait_send()

    def sent_slab(at_send, carry):
        h = at_send // copies
        r = lax.rem(at_send, copies)
        chip, target, copy = slab_copy(h, r, me)

        @pl.when(jnp.logical_not((chip == me) & (target == tp)))
        def _():
            copy.wait_send()

        return carry

    lax.fori_loop(0, heads * copies, sent_slab, 0)

    def sent_fwd(k, carry):
        fwd_copy(2 * k + core).wait_send()
        return carry

    lax.fori_loop(0, n_sp // 2, sent_fwd, 0)

    def sent_att(k, carry):
        j = tile_of(k)
        for p in range(per_tile):
            owner, copy = att_copy(j * per_tile + p, k * per_tile + p)

            @pl.when(jnp.logical_not((owner == me) & (src_tp == tp)))
            def _():
                copy.wait_send()

        return carry

    lax.fori_loop(0, rounds, sent_att, 0)


def on_device(n_sp, n_tp, tokens, wq, wk, wv, q_gain, k_gain, gates, wo):
    own_rows, model = tokens.shape
    shard_rows, heads = gates.shape
    width = wq.shape[1]
    size = width // heads
    copies = n_sp // (2 * heads)
    total = n_sp * shard_rows
    tile, block = 256, 512
    rounds = total // tile // (2 * copies)
    slab_rows = 3 * size + 2 * GATE_ROWS
    per_tile = tile // LANES
    per_chunk = shard_rows // LANES
    hbm = pl.BlockSpec(memory_space=pl.ANY)
    vmem = pl.BlockSpec(memory_space=pltpu.VMEM)
    dma = pltpu.SemaphoreType.DMA
    return pl.pallas_call(
        functools.partial(kernel, n_sp, n_tp, heads, size, shard_rows, tile, block),
        out_shape=jax.ShapeDtypeStruct((own_rows, model), BF16),
        in_specs=[hbm, hbm, hbm, hbm, vmem, vmem, vmem, hbm],
        out_specs=vmem,
        scratch_shapes=[
            pltpu.VMEM((n_tp, own_rows, model), BF16),
            pltpu.VMEM(wq.shape, BF16),
            pltpu.VMEM(wk.shape, BF16),
            pltpu.VMEM(wv.shape, BF16),
            pltpu.VMEM(wo.shape, BF16),
            pltpu.VMEM((heads, slab_rows, shard_rows), BF16),
            pltpu.VMEM((n_sp, slab_rows, shard_rows), BF16),
            pltpu.VMEM((total, LANES), BF16),
            pltpu.VMEM((size, total), BF16),
            pltpu.VMEM((rounds * per_tile, size, LANES), BF16),
            pltpu.VMEM((heads, per_chunk, size, LANES), BF16),
            pltpu.VMEM((shard_rows, width), BF16),
            pltpu.VMEM((n_tp, own_rows, model), BF16),
            pltpu.VMEM((n_tp, own_rows, model), BF16),
            dma((5,)),
            dma((n_tp,)),
            dma((n_tp,)),
            dma((heads * copies,)),
            dma((n_sp,)),
            dma((n_sp,)),
            dma((rounds * per_tile,)),
            dma((heads * per_chunk,)),
            dma((n_tp,)),
            dma((n_tp,)),
        ],
        compiler_params=pltpu.CompilerParams(
            has_side_effects=True, vmem_limit_bytes=60 * 1024 * 1024
        ),
    )(
        tokens, wq, wk, wv,
        (q_gain * size ** (-0.5)).reshape(size, 1), k_gain.reshape(size, 1),
        gates.T, wo,
    )


def solution(mesh):
    placed = (
        P(("sp", "tp"), None),
        P(None, "tp"),
        P(None, "tp"),
        P(None, "tp"),
        P(),
        P(),
        P("sp", "tp"),
        P("tp", None),
    )
    return jax.shard_map(
        functools.partial(on_device, mesh.shape["sp"], mesh.shape["tp"]),
        mesh=mesh, in_specs=placed, out_specs=P(("sp", "tp"), None), check_vma=False,
    )
```

```python
import functools
import math

import jax
import jax.numpy as jnp
from jax import lax
from jax.experimental import pallas as pl
from jax.experimental.pallas import tpu as pltpu
from jax.sharding import PartitionSpec as P

NORM_EPS = 1e-06
LANES = 128
GATE_ROWS = 16
F32 = jnp.float32
BF16 = jnp.bfloat16
MESH = pl.DeviceIdType.MESH


def split3(value):
    first = value.astype(BF16).astype(F32)
    rest = value - first
    second = rest.astype(BF16).astype(F32)
    third = (rest - second).astype(BF16).astype(F32)
    return first, second, third


def kernel(
    n_sp, n_tp, heads, size, shard_rows, tile, block,
    tok_ref, wq_ref, wk_ref, wv_ref, qg_ref, kg_ref, gate_ref, wo_ref,
    out_ref,
    tok_all, wq, wk, wv, wo, stage, slab, kbuf, vbuf, att_stage, att_all, att_rows, part, part_in, even, odd,
    w_sem, tok_send, tok_recv, slab_send, slab_recv, fwd_send, att_send, att_recv, part_send, part_recv,
):
    me = lax.axis_index("sp")
    tp = lax.axis_index("tp")
    core = lax.rem(tp, 2)
    pair = tp - core
    own_rows = tok_ref.shape[0]
    width = heads * size
    copies = n_sp // (2 * heads)
    k_row = size + GATE_ROWS
    v_row = 2 * k_row
    head_of_chip = me // copies
    src_tp = pair + head_of_chip // heads
    src_head = lax.rem(head_of_chip, heads)
    rank = lax.rem(me, copies) * 2 + core
    group = 2 * copies
    tokens_total = n_sp * shard_rows
    rounds = tokens_total // tile // group
    per_tile = tile // LANES
    per_chunk = shard_rows // LANES

    barrier = pltpu.get_barrier_semaphore()

    def greet(chip, carry):
        for side in range(2):
            @pl.when(jnp.logical_not((chip == me) & (side == core)))
            def _():
                pl.semaphore_signal(barrier, inc=1, device_id=(chip, pair + side), device_id_type=MESH)

        return carry

    lax.fori_loop(0, n_sp, greet, 0)
    for step in range(2, n_tp):
        pl.semaphore_signal(
            barrier, inc=1, device_id=(me, lax.rem(pair + step, n_tp)), device_id_type=MESH
        )

    loads = [
        pltpu.make_async_copy(src, dst, w_sem.at[at])
        for at, (src, dst) in enumerate(
            ((wq_ref, wq), (wk_ref, wk), (wv_ref, wv), (wo_ref, wo), (tok_ref, tok_all.at[tp]))
        )
    ]

    def tok_copy(step):
        peer = lax.rem(tp + step, n_tp)
        return pltpu.make_async_remote_copy(
            src_ref=tok_ref, dst_ref=tok_all.at[tp],
            send_sem=tok_send.at[step], recv_sem=tok_recv.at[step],
            device_id=(me, peer), device_id_type=MESH,
        )

    tok_copies = [tok_copy(step) for step in range(1, n_tp)]
    loads[4].start()
    for load in loads[:4]:
        load.start()

    row = lax.broadcasted_iota(jnp.int32, (GATE_ROWS, shard_rows), 0)
    for h in range(heads):
        a, b, c = split3(gate_ref[h : h + 1, :])
        one = jnp.ones((GATE_ROWS, shard_rows), F32)
        zero = jnp.zeros((GATE_ROWS, shard_rows), F32)
        first = jnp.where(row == 0, a, jnp.where(row == 1, b, jnp.where(row == 2, c, zero)))
        k_side = jnp.where((row >= 3) & (row < 6), one, first)
        later = jnp.where(row == 3, a, jnp.where(row == 4, b, jnp.where(row == 5, c, zero)))
        q_side = jnp.where(row < 3, -one, later)
        stage[h, size : size + GATE_ROWS, :] = q_side.astype(BF16)
        stage[h, k_row + size : k_row + size + GATE_ROWS, :] = k_side.astype(BF16)

    eye = lax.broadcasted_iota(jnp.int32, (size, size), 0) == lax.broadcasted_iota(
        jnp.int32, (size, size), 1
    )

    def column(ref):
        return jnp.sum(jnp.where(eye, ref[...], 0.0), axis=1, keepdims=True)

    q_gain = column(qg_ref) * size ** (-0.5)
    k_gain = column(kg_ref)

    pl.semaphore_wait(barrier, 2 * n_sp - 1 + n_tp - 2)
    for copy in tok_copies:
        copy.start()
    loads[4].wait()
    for copy in tok_copies:
        copy.wait()

    def slab_copy(h, r, source):
        chip = (core * heads + h) * copies + r
        target = pair + lax.rem(source, 2)
        return chip, target, pltpu.make_async_remote_copy(
            src_ref=stage.at[h], dst_ref=slab.at[source],
            send_sem=slab_send.at[h * copies + r], recv_sem=slab_recv.at[source],
            device_id=(chip, target), device_id_type=MESH,
        )

    def slab_local(h):
        return pltpu.make_async_copy(stage.at[h], slab.at[me], slab_recv.at[me])

    for load in loads[:3]:
        load.wait()

    cols = math.gcd(width, 256)
    group_heads = cols // size

    def project(j, carry):
        at = pl.ds(pl.multiple_of(j * cols, cols), cols)
        for base, weight, gain in ((0, wq, q_gain), (k_row, wk, k_gain), (v_row, wv, None)):
            raw = jnp.dot(
                tok_all[...].reshape(n_tp * own_rows, tok_all.shape[2]), weight[:, at],
                preferred_element_type=F32,
            )
            flat = raw.T
            for g in range(group_heads):
                part_t = flat[g * size : (g + 1) * size, :]
                if gain is not None:
                    mean = jnp.mean(part_t * part_t, axis=0, keepdims=True)
                    part_t = part_t * lax.rsqrt(mean + NORM_EPS) * gain
                stage[j * group_heads + g, base : base + size, :] = part_t.astype(BF16)

        def send(at_send, carry):
            h = j * group_heads + at_send // copies
            r = lax.rem(at_send, copies)
            chip, target, copy = slab_copy(h, r, me)
            mine = (chip == me) & (target == tp)

            @pl.when(jnp.logical_not(mine))
            def _():
                copy.start()

            @pl.when(mine)
            def _():
                slab_local(h).start()

            return carry

        lax.fori_loop(0, group_heads * copies, send, 0)
        return carry

    lax.fori_loop(0, width // cols, project, 0)

    def fwd_copy(source):
        return pltpu.make_async_remote_copy(
            src_ref=slab.at[source], dst_ref=slab.at[source],
            send_sem=fwd_send.at[source], recv_sem=slab_recv.at[source],
            device_id=(me, pair + 1 - core), device_id_type=MESH,
        )

    def take(k, carry):
        source = 2 * k + core
        fwd_copy(source).wait_recv()
        fwd_copy(source).start()
        return carry

    lax.fori_loop(0, n_sp // 2, take, 0)

    def take_sibling(k, carry):
        fwd_copy(2 * k + 1 - core).wait_recv()
        return carry

    lax.fori_loop(0, n_sp // 2, take_sibling, 0)

    def prepare(i, carry):
        at = pl.ds(pl.multiple_of(i * shard_rows, shard_rows), shard_rows)
        kbuf[at, :] = slab[i, k_row : k_row + LANES, :].T
        vbuf[:, at] = slab[i, v_row : v_row + size, :]
        return carry

    lax.fori_loop(0, n_sp, prepare, 0)

    def att_copy(g, slot):
        owner = g // per_chunk
        where_to = lax.rem(g, per_chunk)
        return owner, pltpu.make_async_remote_copy(
            src_ref=att_stage.at[slot], dst_ref=att_all.at[src_head, where_to],
            send_sem=att_send.at[slot], recv_sem=att_recv.at[src_head * per_chunk + where_to],
            device_id=(owner, src_tp), device_id_type=MESH,
        )

    def att_local(g, slot):
        where_to = lax.rem(g, per_chunk)
        return pltpu.make_async_copy(
            att_stage.at[slot], att_all.at[src_head, where_to],
            att_recv.at[src_head * per_chunk + where_to],
        )

    def tile_of(k):
        return k * group + jnp.where(lax.rem(k, 2) == 0, rank, group - 1 - rank)

    def attend(k, carry):
        j = tile_of(k)
        pieces = []
        for p in range(per_tile):
            g = j * per_tile + p
            lane = pl.ds(pl.multiple_of(lax.rem(g, per_chunk) * LANES, LANES), LANES)
            pieces.append(slab[g // per_chunk, 0:k_row, lane])
        q = jnp.concatenate(pieces, axis=1)
        q = jnp.concatenate([q, jnp.zeros((LANES - k_row, tile), BF16)], axis=0)

        def produce(ref, i, masked=False):
            at = pl.ds(pl.multiple_of(i * block, block), block)
            s = jnp.dot(kbuf[at, :], q, preferred_element_type=F32)
            if masked:
                key = i * block + lax.broadcasted_iota(jnp.int32, (block, tile), 0)
                query = j * tile + lax.broadcasted_iota(jnp.int32, (block, tile), 1)
                s = jnp.where(key <= query, s, -jnp.inf)
            ref[...] = s
            return jnp.max(s, axis=0, keepdims=True)

        def consume(ref, highest, i, state):
            top, total, acc = state
            at = pl.ds(pl.multiple_of(i * block, block), block)
            new_top = jnp.maximum(top, highest)
            p = jnp.exp(ref[...] - new_top)
            scale = jnp.exp(top - new_top)
            total = total * scale + jnp.sum(p, axis=0, keepdims=True)
            acc = acc * scale + jnp.dot(vbuf[:, at], p.astype(BF16), preferred_element_type=F32)
            return new_top, total, acc

        state = (
            jnp.full((1, tile), -1e30, F32),
            jnp.zeros((1, tile), F32),
            jnp.zeros((size, tile), F32),
        )
        full = j * tile // block
        high = produce(even, full, True)
        high_next = produce(odd, 0)
        state = consume(even, high, full, state)

        def two(i, carry):
            high, state = carry
            high_next = produce(even, 2 * i + 1)
            state = consume(odd, high, 2 * i, state)
            high = produce(odd, 2 * i + 2)
            state = consume(even, high_next, 2 * i + 1, state)
            return high, state

        pairs = full // 2
        high, state = lax.fori_loop(0, pairs, two, (high_next, state))
        top, total, acc = lax.fori_loop(
            2 * pairs, full, lambda i, st: consume(odd, high, i, st), state
        )
        done = (acc / total).astype(BF16)
        for p in range(per_tile):
            slot = k * per_tile + p
            att_stage[slot] = done[:, p * LANES : (p + 1) * LANES]
        for p in range(per_tile):
            slot = k * per_tile + p
            g = j * per_tile + p
            owner, copy = att_copy(g, slot)
            mine = (owner == me) & (src_tp == tp)

            @pl.when(jnp.logical_not(mine))
            def _():
                copy.start()

            @pl.when(mine)
            def _():
                att_local(g, slot).start()

        return carry

    lax.fori_loop(0, rounds, attend, 0)

    loads[3].wait()

    def att_wait(at, carry):
        h = at // per_chunk
        p = lax.rem(at, per_chunk)
        pltpu.make_async_remote_copy(
            src_ref=att_stage.at[0], dst_ref=att_all.at[h, p],
            send_sem=att_send.at[0], recv_sem=att_recv.at[at],
            device_id=(me, pair + 1 - core), device_id_type=MESH,
        ).wait_recv()
        return carry

    lax.fori_loop(0, heads * per_chunk, att_wait, 0)
    for p in range(per_chunk):
        joined = jnp.concatenate([att_all[h, p] for h in range(heads)], axis=0)
        att_rows[p * LANES : (p + 1) * LANES, :] = joined.T

    def part_copy(step):
        peer = lax.rem(tp + step, n_tp)
        return pltpu.make_async_remote_copy(
            src_ref=part.at[peer], dst_ref=part_in.at[step],
            send_sem=part_send.at[step], recv_sem=part_recv.at[step],
            device_id=(me, peer), device_id_type=MESH,
        )

    model = wo.shape[1]
    out_cols = math.gcd(model, 512)

    def project_rows(step, carry):
        peer = lax.rem(tp + step, n_tp)
        rows = att_rows[pl.ds(pl.multiple_of(peer * own_rows, math.gcd(own_rows, LANES)), own_rows), :]

        def columns(c, carry):
            at = pl.ds(pl.multiple_of(c * out_cols, out_cols), out_cols)
            part[peer, :, at] = jnp.dot(rows, wo[:, at], preferred_element_type=F32).astype(BF16)
            return carry

        lax.fori_loop(0, model // out_cols, columns, 0)
        return carry

    for step in range(1, n_tp):
        project_rows(step, 0)
        part_copy(step).start()
    project_rows(0, 0)
    for step in range(1, n_tp):
        part_copy(step).wait_recv()

    def finish(c, carry):
        at = pl.ds(pl.multiple_of(c * out_cols, out_cols), out_cols)
        mixed = part[tp, :, at].astype(F32)
        for step in range(1, n_tp):
            mixed = mixed + part_in[step, :, at].astype(F32)
        out_ref[:, at] = mixed.astype(BF16)
        return carry

    lax.fori_loop(0, model // out_cols, finish, 0)

    for step in range(1, n_tp):
        part_copy(step).wait_send()

    def sent_slab(at_send, carry):
        h = at_send // copies
        r = lax.rem(at_send, copies)
        chip, target, copy = slab_copy(h, r, me)

        @pl.when(jnp.logical_not((chip == me) & (target == tp)))
        def _():
            copy.wait_send()

        return carry

    lax.fori_loop(0, heads * copies, sent_slab, 0)

    def sent_fwd(k, carry):
        fwd_copy(2 * k + core).wait_send()
        return carry

    lax.fori_loop(0, n_sp // 2, sent_fwd, 0)

    def sent_att(k, carry):
        j = tile_of(k)
        for p in range(per_tile):
            owner, copy = att_copy(j * per_tile + p, k * per_tile + p)

            @pl.when(jnp.logical_not((owner == me) & (src_tp == tp)))
            def _():
                copy.wait_send()

        return carry

    lax.fori_loop(0, rounds, sent_att, 0)


def on_device(n_sp, n_tp, tokens, wq, wk, wv, q_gain, k_gain, gates, wo):
    own_rows, model = tokens.shape
    shard_rows, heads = gates.shape
    width = wq.shape[1]
    size = width // heads
    copies = n_sp // (2 * heads)
    total = n_sp * shard_rows
    tile, block = 256, 1024
    rounds = total // tile // (2 * copies)
    slab_rows = 3 * size + 2 * GATE_ROWS
    per_tile = tile // LANES
    per_chunk = shard_rows // LANES
    hbm = pl.BlockSpec(memory_space=pl.ANY)
    vmem = pl.BlockSpec(memory_space=pltpu.VMEM)
    dma = pltpu.SemaphoreType.DMA
    return pl.pallas_call(
        functools.partial(kernel, n_sp, n_tp, heads, size, shard_rows, tile, block),
        out_shape=jax.ShapeDtypeStruct((own_rows, model), BF16),
        in_specs=[hbm, hbm, hbm, hbm, vmem, vmem, vmem, hbm],
        out_specs=vmem,
        scratch_shapes=[
            pltpu.VMEM((n_tp, own_rows, model), BF16),
            pltpu.VMEM(wq.shape, BF16),
            pltpu.VMEM(wk.shape, BF16),
            pltpu.VMEM(wv.shape, BF16),
            pltpu.VMEM(wo.shape, BF16),
            pltpu.VMEM((heads, slab_rows, shard_rows), BF16),
            pltpu.VMEM((n_sp, slab_rows, shard_rows), BF16),
            pltpu.VMEM((total, LANES), BF16),
            pltpu.VMEM((size, total), BF16),
            pltpu.VMEM((rounds * per_tile, size, LANES), BF16),
            pltpu.VMEM((heads, per_chunk, size, LANES), BF16),
            pltpu.VMEM((shard_rows, width), BF16),
            pltpu.VMEM((n_tp, own_rows, model), BF16),
            pltpu.VMEM((n_tp, own_rows, model), BF16),
            pltpu.VMEM((block, tile), F32),
            pltpu.VMEM((block, tile), F32),
            dma((5,)),
            dma((n_tp,)),
            dma((n_tp,)),
            dma((heads * copies,)),
            dma((n_sp,)),
            dma((n_sp,)),
            dma((rounds * per_tile,)),
            dma((heads * per_chunk,)),
            dma((n_tp,)),
            dma((n_tp,)),
        ],
        compiler_params=pltpu.CompilerParams(
            has_side_effects=True, collective_id=0, vmem_limit_bytes=60 * 1024 * 1024
        ),
    )(
        tokens, wq, wk, wv,
        q_gain.reshape(1, size), k_gain.reshape(1, size),
        gates.T, wo,
    )


def solution(mesh):
    placed = (
        P(("sp", "tp"), None),
        P(None, "tp"),
        P(None, "tp"),
        P(None, "tp"),
        P(),
        P(),
        P("sp", "tp"),
        P("tp", None),
    )
    return jax.shard_map(
        functools.partial(on_device, mesh.shape["sp"], mesh.shape["tp"]),
        mesh=mesh, in_specs=placed, out_specs=P(("sp", "tp"), None), check_vma=False,
    )
```

```python
import functools
import math

import jax
import jax.numpy as jnp
from jax import lax
from jax.experimental import pallas as pl
from jax.experimental.pallas import tpu as pltpu
from jax.sharding import PartitionSpec as P

NORM_EPS = 1e-06
LANES = 128
GATE_ROWS = 16
F32 = jnp.float32
BF16 = jnp.bfloat16
MESH = pl.DeviceIdType.MESH


def split3(value):
    first = value.astype(BF16).astype(F32)
    rest = value - first
    second = rest.astype(BF16).astype(F32)
    third = (rest - second).astype(BF16).astype(F32)
    return first, second, third


def kernel(
    n_sp, n_tp, heads, size, shard_rows, tile, block,
    tok_ref, wq_ref, wk_ref, wv_ref, qg_ref, kg_ref, gate_ref, wo_ref,
    out_ref,
    tok_all, wq, wk, wv, wo, stage, slab, kbuf, vbuf, att_stage, att_all, att_rows, part, part_in, even, odd, kept_top, kept_total, kept_acc,
    w_sem, tok_send, tok_recv, slab_send, slab_recv, fwd_send, att_send, att_recv, part_send, part_recv,
):
    me = lax.axis_index("sp")
    tp = lax.axis_index("tp")
    core = lax.rem(tp, 2)
    pair = tp - core
    own_rows = tok_ref.shape[0]
    width = heads * size
    copies = n_sp // (2 * heads)
    k_row = size
    gate_row = 2 * size
    v_row = gate_row + GATE_ROWS
    head_of_chip = me // copies
    src_tp = pair + head_of_chip // heads
    src_head = lax.rem(head_of_chip, heads)
    rank = lax.rem(me, copies) * 2 + core
    group = 2 * copies
    tokens_total = n_sp * shard_rows
    rounds = tokens_total // tile // group
    per_tile = tile // LANES
    per_chunk = shard_rows // LANES

    barrier = pltpu.get_barrier_semaphore()

    def greet(chip, carry):
        for side in range(2):
            @pl.when(jnp.logical_not((chip == me) & (side == core)))
            def _():
                pl.semaphore_signal(barrier, inc=1, device_id=(chip, pair + side), device_id_type=MESH)

        return carry

    lax.fori_loop(0, n_sp, greet, 0)
    for step in range(2, n_tp):
        pl.semaphore_signal(
            barrier, inc=1, device_id=(me, lax.rem(pair + step, n_tp)), device_id_type=MESH
        )

    loads = [
        pltpu.make_async_copy(src, dst, w_sem.at[at])
        for at, (src, dst) in enumerate(
            ((wq_ref, wq), (wk_ref, wk), (wv_ref, wv), (wo_ref, wo), (tok_ref, tok_all.at[tp]))
        )
    ]

    def tok_copy(step):
        peer = lax.rem(tp + step, n_tp)
        return pltpu.make_async_remote_copy(
            src_ref=tok_ref, dst_ref=tok_all.at[tp],
            send_sem=tok_send.at[step], recv_sem=tok_recv.at[step],
            device_id=(me, peer), device_id_type=MESH,
        )

    tok_copies = [tok_copy(step) for step in range(1, n_tp)]
    loads[4].start()
    for load in loads[:4]:
        load.start()

    row = lax.broadcasted_iota(jnp.int32, (GATE_ROWS, shard_rows), 0)
    for h in range(heads):
        a, b, c = split3(gate_ref[h : h + 1, :])
        one = jnp.ones((GATE_ROWS, shard_rows), F32)
        zero = jnp.zeros((GATE_ROWS, shard_rows), F32)
        first = jnp.where(row == 0, a, jnp.where(row == 1, b, jnp.where(row == 2, c, zero)))
        k_side = jnp.where((row >= 3) & (row < 6), one, first)
        stage[h, gate_row : gate_row + GATE_ROWS, :] = k_side.astype(BF16)

    eye = lax.broadcasted_iota(jnp.int32, (size, size), 0) == lax.broadcasted_iota(
        jnp.int32, (size, size), 1
    )

    def column(ref):
        return jnp.sum(jnp.where(eye, ref[...], 0.0), axis=1, keepdims=True)

    q_gain = column(qg_ref) * size ** (-0.5)
    k_gain = column(kg_ref)

    pl.semaphore_wait(barrier, 2 * n_sp - 1 + n_tp - 2)
    for copy in tok_copies:
        copy.start()
    loads[4].wait()
    for copy in tok_copies:
        copy.wait()

    def slab_copy(h, r, source):
        chip = (core * heads + h) * copies + r
        target = pair + lax.rem(source, 2)
        return chip, target, pltpu.make_async_remote_copy(
            src_ref=stage.at[h], dst_ref=slab.at[source],
            send_sem=slab_send.at[h * copies + r], recv_sem=slab_recv.at[source],
            device_id=(chip, target), device_id_type=MESH,
        )

    def slab_local(h):
        return pltpu.make_async_copy(stage.at[h], slab.at[me], slab_recv.at[me])

    for load in loads[:3]:
        load.wait()

    cols = math.gcd(width, 256)
    group_heads = cols // size

    def project(j, carry):
        at = pl.ds(pl.multiple_of(j * cols, cols), cols)
        for base, weight, gain in ((0, wq, q_gain), (k_row, wk, k_gain), (v_row, wv, None)):
            raw = jnp.dot(
                tok_all[...].reshape(n_tp * own_rows, tok_all.shape[2]), weight[:, at],
                preferred_element_type=F32,
            )
            flat = raw.T
            for g in range(group_heads):
                part_t = flat[g * size : (g + 1) * size, :]
                if gain is not None:
                    mean = jnp.mean(part_t * part_t, axis=0, keepdims=True)
                    part_t = part_t * lax.rsqrt(mean + NORM_EPS) * gain
                stage[j * group_heads + g, base : base + size, :] = part_t.astype(BF16)

        def send(at_send, carry):
            h = j * group_heads + at_send // copies
            r = lax.rem(at_send, copies)
            chip, target, copy = slab_copy(h, r, me)
            mine = (chip == me) & (target == tp)

            @pl.when(jnp.logical_not(mine))
            def _():
                copy.start()

            @pl.when(mine)
            def _():
                slab_local(h).start()

            return carry

        lax.fori_loop(0, group_heads * copies, send, 0)
        return carry

    lax.fori_loop(0, width // cols, project, 0)

    def fwd_copy(source):
        return pltpu.make_async_remote_copy(
            src_ref=slab.at[source], dst_ref=slab.at[source],
            send_sem=fwd_send.at[source], recv_sem=slab_recv.at[source],
            device_id=(me, pair + 1 - core), device_id_type=MESH,
        )

    half = n_sp // 2
    upper = me >= half

    def take_half(first):
        def take(k, carry):
            source = first + 2 * k + core
            fwd_copy(source).wait_recv()
            fwd_copy(source).start()
            return carry

        lax.fori_loop(0, half // 2, take, 0)

        def take_sibling(k, carry):
            fwd_copy(first + 2 * k + 1 - core).wait_recv()
            return carry

        lax.fori_loop(0, half // 2, take_sibling, 0)

        def prepare(k, carry):
            i = first + k
            at = pl.ds(pl.multiple_of(i * shard_rows, shard_rows), shard_rows)
            kbuf[at, :] = slab[i, k_row : k_row + LANES, :].T
            vbuf[:, at] = slab[i, v_row : v_row + size, :]
            return carry

        lax.fori_loop(0, half, prepare, 0)

    def att_copy(g, slot):
        owner = g // per_chunk
        where_to = lax.rem(g, per_chunk)
        return owner, pltpu.make_async_remote_copy(
            src_ref=att_stage.at[slot], dst_ref=att_all.at[src_head, where_to],
            send_sem=att_send.at[slot], recv_sem=att_recv.at[src_head * per_chunk + where_to],
            device_id=(owner, src_tp), device_id_type=MESH,
        )

    def att_local(g, slot):
        where_to = lax.rem(g, per_chunk)
        return pltpu.make_async_copy(
            att_stage.at[slot], att_all.at[src_head, where_to],
            att_recv.at[src_head * per_chunk + where_to],
        )

    def tile_of(k):
        return k * group + jnp.where(lax.rem(k, 2) == 0, rank, group - 1 - rank)

    half_tiles = tokens_total // tile // 2
    half_blocks = tokens_total // block // 2

    def attend(k, second):
        j = tile_of(k)
        near = (j >= half_tiles) == upper
        pieces, gates = [], []
        for p in range(per_tile):
            g = j * per_tile + p
            lane = pl.ds(pl.multiple_of(lax.rem(g, per_chunk) * LANES, LANES), LANES)
            pieces.append(slab[g // per_chunk, 0:size, lane])
            gates.append(slab[g // per_chunk, gate_row : gate_row + GATE_ROWS, lane])
        q_gate = jnp.concatenate(gates, axis=1).astype(F32)
        line = lax.broadcasted_iota(jnp.int32, (GATE_ROWS, tile), 0)
        mixed_gate = jnp.where(line < 3, -1.0, 0.0)
        for n in range(3):
            mixed_gate = jnp.where(line == 3 + n, q_gate[n : n + 1, :], mixed_gate)
        q = jnp.concatenate(
            [
                jnp.concatenate(pieces, axis=1),
                mixed_gate.astype(BF16),
                jnp.zeros((LANES - size - GATE_ROWS, tile), BF16),
            ],
            axis=0,
        )

        def produce(ref, i, masked=False):
            at = pl.ds(pl.multiple_of(i * block, block), block)
            s = jnp.dot(kbuf[at, :], q, preferred_element_type=F32)
            if masked:
                key = i * block + lax.broadcasted_iota(jnp.int32, (block, tile), 0)
                query = j * tile + lax.broadcasted_iota(jnp.int32, (block, tile), 1)
                s = jnp.where(key <= query, s, -jnp.inf)
            ref[...] = s
            return jnp.max(s, axis=0, keepdims=True)

        def consume(ref, highest, i, state):
            top, total, acc = state
            at = pl.ds(pl.multiple_of(i * block, block), block)
            new_top = jnp.maximum(top, highest)
            p = jnp.exp(ref[...] - new_top)
            scale = jnp.exp(top - new_top)
            total = total * scale + jnp.sum(p, axis=0, keepdims=True)
            acc = acc * scale + jnp.dot(vbuf[:, at], p.astype(BF16), preferred_element_type=F32)
            return new_top, total, acc

        fresh = (
            jnp.full((1, tile), -1e30, F32),
            jnp.zeros((1, tile), F32),
            jnp.zeros((size, tile), F32),
        )
        full = j * tile // block

        def save(state):
            kept_top[k], kept_total[k], kept_acc[k] = state

        if second:
            low = 0
            high_end = jnp.where(near, half_blocks, full)

            @pl.when(jnp.logical_not(near))
            def _():
                high = produce(even, full, True)
                save(consume(even, high, full, fresh))

            high_next = produce(odd, low)
            state = (kept_top[k], kept_total[k], kept_acc[k])
        else:
            low = jnp.where(upper, half_blocks, 0)
            high_end = full
            high = produce(even, full, True)
            high_next = produce(odd, low)
            state = consume(even, high, full, fresh)

        def two(i, carry):
            high, state = carry
            high_next = produce(even, low + 2 * i + 1)
            state = consume(odd, high, low + 2 * i, state)
            high = produce(odd, low + 2 * i + 2)
            state = consume(even, high_next, low + 2 * i + 1, state)
            return high, state

        pairs = (high_end - low) // 2
        high, state = lax.fori_loop(0, pairs, two, (high_next, state))
        state = lax.fori_loop(
            low + 2 * pairs, high_end, lambda i, st: consume(odd, high, i, st), state
        )
        if second:
            emit(k, j, state)
        else:
            pl.when(upper)(lambda: save(state))
            pl.when(jnp.logical_not(upper))(lambda: emit(k, j, state))

    def emit(k, j, state):
        top, total, acc = state
        done = (acc / total).astype(BF16)
        for p in range(per_tile):
            slot = k * per_tile + p
            att_stage[slot] = done[:, p * LANES : (p + 1) * LANES]
        for p in range(per_tile):
            slot = k * per_tile + p
            g = j * per_tile + p
            owner, copy = att_copy(g, slot)
            mine = (owner == me) & (src_tp == tp)

            @pl.when(jnp.logical_not(mine))
            def _():
                copy.start()

            @pl.when(mine)
            def _():
                att_local(g, slot).start()

    def first_pass(k, carry):
        pl.when((tile_of(k) >= half_tiles) == upper)(lambda: attend(k, False))
        return carry

    def second_pass(k, carry):
        pl.when(upper | (tile_of(k) >= half_tiles))(lambda: attend(k, True))
        return carry

    take_half(jnp.where(upper, half, 0))
    lax.fori_loop(0, rounds, first_pass, 0)
    take_half(jnp.where(upper, 0, half))
    lax.fori_loop(0, rounds, second_pass, 0)

    loads[3].wait()

    def att_wait(at, carry):
        h = at // per_chunk
        p = lax.rem(at, per_chunk)
        pltpu.make_async_remote_copy(
            src_ref=att_stage.at[0], dst_ref=att_all.at[h, p],
            send_sem=att_send.at[0], recv_sem=att_recv.at[at],
            device_id=(me, pair + 1 - core), device_id_type=MESH,
        ).wait_recv()
        return carry

    lax.fori_loop(0, heads * per_chunk, att_wait, 0)
    for p in range(per_chunk):
        joined = jnp.concatenate([att_all[h, p] for h in range(heads)], axis=0)
        att_rows[p * LANES : (p + 1) * LANES, :] = joined.T

    def part_copy(step):
        peer = lax.rem(tp + step, n_tp)
        return pltpu.make_async_remote_copy(
            src_ref=part.at[peer], dst_ref=part_in.at[step],
            send_sem=part_send.at[step], recv_sem=part_recv.at[step],
            device_id=(me, peer), device_id_type=MESH,
        )

    model = wo.shape[1]
    out_cols = math.gcd(model, 512)

    def project_rows(step, carry):
        peer = lax.rem(tp + step, n_tp)
        rows = att_rows[pl.ds(pl.multiple_of(peer * own_rows, math.gcd(own_rows, LANES)), own_rows), :]

        def columns(c, carry):
            at = pl.ds(pl.multiple_of(c * out_cols, out_cols), out_cols)
            part[peer, :, at] = jnp.dot(rows, wo[:, at], preferred_element_type=F32).astype(BF16)
            return carry

        lax.fori_loop(0, model // out_cols, columns, 0)
        return carry

    for step in range(1, n_tp):
        project_rows(step, 0)
        part_copy(step).start()
    project_rows(0, 0)
    for step in range(1, n_tp):
        part_copy(step).wait_recv()

    def finish(c, carry):
        at = pl.ds(pl.multiple_of(c * out_cols, out_cols), out_cols)
        mixed = part[tp, :, at].astype(F32)
        for step in range(1, n_tp):
            mixed = mixed + part_in[step, :, at].astype(F32)
        out_ref[:, at] = mixed.astype(BF16)
        return carry

    lax.fori_loop(0, model // out_cols, finish, 0)

    for step in range(1, n_tp):
        part_copy(step).wait_send()

    def sent_slab(at_send, carry):
        h = at_send // copies
        r = lax.rem(at_send, copies)
        chip, target, copy = slab_copy(h, r, me)

        @pl.when(jnp.logical_not((chip == me) & (target == tp)))
        def _():
            copy.wait_send()

        return carry

    lax.fori_loop(0, heads * copies, sent_slab, 0)

    def sent_fwd(k, carry):
        fwd_copy(2 * k + core).wait_send()
        return carry

    lax.fori_loop(0, n_sp // 2, sent_fwd, 0)

    def sent_att(k, carry):
        j = tile_of(k)
        for p in range(per_tile):
            owner, copy = att_copy(j * per_tile + p, k * per_tile + p)

            @pl.when(jnp.logical_not((owner == me) & (src_tp == tp)))
            def _():
                copy.wait_send()

        return carry

    lax.fori_loop(0, rounds, sent_att, 0)


def on_device(n_sp, n_tp, tokens, wq, wk, wv, q_gain, k_gain, gates, wo):
    own_rows, model = tokens.shape
    shard_rows, heads = gates.shape
    width = wq.shape[1]
    size = width // heads
    copies = n_sp // (2 * heads)
    total = n_sp * shard_rows
    tile, block = 256, 1024
    rounds = total // tile // (2 * copies)
    slab_rows = 3 * size + GATE_ROWS
    per_tile = tile // LANES
    per_chunk = shard_rows // LANES
    hbm = pl.BlockSpec(memory_space=pl.ANY)
    vmem = pl.BlockSpec(memory_space=pltpu.VMEM)
    dma = pltpu.SemaphoreType.DMA
    return pl.pallas_call(
        functools.partial(kernel, n_sp, n_tp, heads, size, shard_rows, tile, block),
        out_shape=jax.ShapeDtypeStruct((own_rows, model), BF16),
        in_specs=[hbm, hbm, hbm, hbm, vmem, vmem, vmem, hbm],
        out_specs=vmem,
        scratch_shapes=[
            pltpu.VMEM((n_tp, own_rows, model), BF16),
            pltpu.VMEM(wq.shape, BF16),
            pltpu.VMEM(wk.shape, BF16),
            pltpu.VMEM(wv.shape, BF16),
            pltpu.VMEM(wo.shape, BF16),
            pltpu.VMEM((heads, slab_rows, shard_rows), BF16),
            pltpu.VMEM((n_sp, slab_rows, shard_rows), BF16),
            pltpu.VMEM((total, LANES), BF16),
            pltpu.VMEM((size, total), BF16),
            pltpu.VMEM((rounds * per_tile, size, LANES), BF16),
            pltpu.VMEM((heads, per_chunk, size, LANES), BF16),
            pltpu.VMEM((shard_rows, width), BF16),
            pltpu.VMEM((n_tp, own_rows, model), BF16),
            pltpu.VMEM((n_tp, own_rows, model), BF16),
            pltpu.VMEM((block, tile), F32),
            pltpu.VMEM((block, tile), F32),
            pltpu.VMEM((rounds, 1, tile), F32),
            pltpu.VMEM((rounds, 1, tile), F32),
            pltpu.VMEM((rounds, size, tile), F32),
            dma((5,)),
            dma((n_tp,)),
            dma((n_tp,)),
            dma((heads * copies,)),
            dma((n_sp,)),
            dma((n_sp,)),
            dma((rounds * per_tile,)),
            dma((heads * per_chunk,)),
            dma((n_tp,)),
            dma((n_tp,)),
        ],
        compiler_params=pltpu.CompilerParams(
            has_side_effects=True, collective_id=0, vmem_limit_bytes=60 * 1024 * 1024
        ),
    )(
        tokens, wq, wk, wv,
        q_gain.reshape(1, size), k_gain.reshape(1, size),
        gates.T, wo,
    )


def solution(mesh):
    placed = (
        P(("sp", "tp"), None),
        P(None, "tp"),
        P(None, "tp"),
        P(None, "tp"),
        P(),
        P(),
        P("sp", "tp"),
        P("tp", None),
    )
    return jax.shard_map(
        functools.partial(on_device, mesh.shape["sp"], mesh.shape["tp"]),
        mesh=mesh, in_specs=placed, out_specs=P(("sp", "tp"), None), check_vma=False,
    )
```

```python
import functools
import math

import jax
import jax.numpy as jnp
from jax import lax
from jax.experimental import pallas as pl
from jax.experimental.pallas import tpu as pltpu
from jax.sharding import PartitionSpec as P

NORM_EPS = 1e-06
LANES = 128
GATE_ROWS = 16
F32 = jnp.float32
BF16 = jnp.bfloat16
MESH = pl.DeviceIdType.MESH


def split3(value):
    first = value.astype(BF16).astype(F32)
    rest = value - first
    second = rest.astype(BF16).astype(F32)
    third = (rest - second).astype(BF16).astype(F32)
    return first, second, third


def kernel(
    n_sp, n_tp, heads, size, shard_rows, tile, block,
    tok_ref, wq_ref, wk_ref, wv_ref, qg_ref, kg_ref, gate_ref, wo_ref,
    out_ref,
    tok_all, wq, wk, wv, wo, stage, slab, kbuf, vbuf, att_stage, att_all, att_rows, part, part_in, even, odd, kept_top, kept_total, kept_acc,
    w_sem, tok_send, tok_recv, slab_send, slab_recv, fwd_send, att_send, att_recv, part_send, part_recv,
):
    me = lax.axis_index("sp")
    tp = lax.axis_index("tp")
    core = lax.rem(tp, 2)
    pair = tp - core
    own_rows = tok_ref.shape[0]
    width = heads * size
    copies = n_sp // (2 * heads)
    k_row = size
    gate_row = 2 * size
    v_row = gate_row + GATE_ROWS
    head_of_chip = me // copies
    src_tp = pair + head_of_chip // heads
    src_head = lax.rem(head_of_chip, heads)
    rank = lax.rem(me, copies) * 2 + core
    group = 2 * copies
    tokens_total = n_sp * shard_rows
    rounds = tokens_total // tile // group
    per_tile = tile // LANES
    per_chunk = shard_rows // LANES

    barrier = pltpu.get_barrier_semaphore()

    def greet(chip, carry):
        for side in range(2):
            @pl.when(jnp.logical_not((chip == me) & (side == core)))
            def _():
                pl.semaphore_signal(barrier, inc=1, device_id=(chip, pair + side), device_id_type=MESH)

        return carry

    lax.fori_loop(0, n_sp, greet, 0)
    for step in range(2, n_tp):
        pl.semaphore_signal(
            barrier, inc=1, device_id=(me, lax.rem(pair + step, n_tp)), device_id_type=MESH
        )

    loads = [
        pltpu.make_async_copy(src, dst, w_sem.at[at])
        for at, (src, dst) in enumerate(
            ((wq_ref, wq), (wk_ref, wk), (wv_ref, wv), (wo_ref, wo), (tok_ref, tok_all.at[tp]))
        )
    ]

    def tok_copy(step):
        peer = lax.rem(tp + step, n_tp)
        return pltpu.make_async_remote_copy(
            src_ref=tok_ref, dst_ref=tok_all.at[tp],
            send_sem=tok_send.at[step], recv_sem=tok_recv.at[step],
            device_id=(me, peer), device_id_type=MESH,
        )

    tok_copies = [tok_copy(step) for step in range(1, n_tp)]
    loads[4].start()
    for load in loads[:4]:
        load.start()

    row = lax.broadcasted_iota(jnp.int32, (GATE_ROWS, shard_rows), 0)
    for h in range(heads):
        a, b, c = split3(gate_ref[h : h + 1, :])
        one = jnp.ones((GATE_ROWS, shard_rows), F32)
        zero = jnp.zeros((GATE_ROWS, shard_rows), F32)
        first = jnp.where(row == 0, a, jnp.where(row == 1, b, jnp.where(row == 2, c, zero)))
        k_side = jnp.where((row >= 3) & (row < 6), one, first)
        stage[h, gate_row : gate_row + GATE_ROWS, :] = k_side.astype(BF16)

    eye = lax.broadcasted_iota(jnp.int32, (size, size), 0) == lax.broadcasted_iota(
        jnp.int32, (size, size), 1
    )

    def column(ref):
        return jnp.sum(jnp.where(eye, ref[...], 0.0), axis=1, keepdims=True)

    q_gain = column(qg_ref) * size ** (-0.5)
    k_gain = column(kg_ref)

    pl.semaphore_wait(barrier, 2 * n_sp - 1 + n_tp - 2)
    for copy in tok_copies:
        copy.start()
    loads[4].wait()
    for copy in tok_copies:
        copy.wait()

    def slab_copy(h, r, source):
        chip = (core * heads + h) * copies + r
        target = pair + lax.rem(source, 2)
        return chip, target, pltpu.make_async_remote_copy(
            src_ref=stage.at[h], dst_ref=slab.at[source],
            send_sem=slab_send.at[h * copies + r], recv_sem=slab_recv.at[source],
            device_id=(chip, target), device_id_type=MESH,
        )

    def slab_local(h):
        return pltpu.make_async_copy(stage.at[h], slab.at[me], slab_recv.at[me])

    for load in loads[:3]:
        load.wait()

    cols = math.gcd(width, 256)
    group_heads = cols // size

    def project(j, carry):
        at = pl.ds(pl.multiple_of(j * cols, cols), cols)
        for base, weight, gain in ((0, wq, q_gain), (k_row, wk, k_gain), (v_row, wv, None)):
            raw = jnp.dot(
                tok_all[...].reshape(n_tp * own_rows, tok_all.shape[2]), weight[:, at],
                preferred_element_type=F32,
            )
            flat = raw.T
            for g in range(group_heads):
                part_t = flat[g * size : (g + 1) * size, :]
                if gain is not None:
                    mean = jnp.mean(part_t * part_t, axis=0, keepdims=True)
                    part_t = part_t * lax.rsqrt(mean + NORM_EPS) * gain
                stage[j * group_heads + g, base : base + size, :] = part_t.astype(BF16)

        def send(at_send, carry):
            h = j * group_heads + lax.rem(at_send // copies + me, group_heads)
            r = lax.rem(at_send, copies)
            chip, target, copy = slab_copy(h, r, me)
            mine = (chip == me) & (target == tp)

            @pl.when(jnp.logical_not(mine))
            def _():
                copy.start()

            @pl.when(mine)
            def _():
                slab_local(h).start()

            return carry

        lax.fori_loop(0, group_heads * copies, send, 0)
        return carry

    lax.fori_loop(0, width // cols, project, 0)

    def fwd_copy(source):
        return pltpu.make_async_remote_copy(
            src_ref=slab.at[source], dst_ref=slab.at[source],
            send_sem=fwd_send.at[source], recv_sem=slab_recv.at[source],
            device_id=(me, pair + 1 - core), device_id_type=MESH,
        )

    half = n_sp // 2
    upper = me >= half

    def take_half(first):
        def take(k, carry):
            source = first + 2 * k + core
            fwd_copy(source).wait_recv()
            fwd_copy(source).start()
            return carry

        lax.fori_loop(0, half // 2, take, 0)

        def take_sibling(k, carry):
            fwd_copy(first + 2 * k + 1 - core).wait_recv()
            return carry

        lax.fori_loop(0, half // 2, take_sibling, 0)

        def prepare(k, carry):
            i = first + k
            at = pl.ds(pl.multiple_of(i * shard_rows, shard_rows), shard_rows)
            kbuf[at, :] = slab[i, k_row : k_row + LANES, :].T
            vbuf[:, at] = slab[i, v_row : v_row + size, :]
            return carry

        lax.fori_loop(0, half, prepare, 0)

    def att_copy(g, slot):
        owner = g // per_chunk
        where_to = lax.rem(g, per_chunk)
        return owner, pltpu.make_async_remote_copy(
            src_ref=att_stage.at[slot], dst_ref=att_all.at[src_head, where_to],
            send_sem=att_send.at[slot], recv_sem=att_recv.at[src_head * per_chunk + where_to],
            device_id=(owner, src_tp), device_id_type=MESH,
        )

    def att_local(g, slot):
        where_to = lax.rem(g, per_chunk)
        return pltpu.make_async_copy(
            att_stage.at[slot], att_all.at[src_head, where_to],
            att_recv.at[src_head * per_chunk + where_to],
        )

    def tile_of(k):
        return k * group + jnp.where(lax.rem(k, 2) == 0, rank, group - 1 - rank)

    half_tiles = tokens_total // tile // 2
    half_blocks = tokens_total // block // 2

    def attend(k, second):
        j = tile_of(k)
        near = (j >= half_tiles) == upper
        pieces, gates = [], []
        for p in range(per_tile):
            g = j * per_tile + p
            lane = pl.ds(pl.multiple_of(lax.rem(g, per_chunk) * LANES, LANES), LANES)
            pieces.append(slab[g // per_chunk, 0:size, lane])
            gates.append(slab[g // per_chunk, gate_row : gate_row + GATE_ROWS, lane])
        q_gate = jnp.concatenate(gates, axis=1).astype(F32)
        line = lax.broadcasted_iota(jnp.int32, (GATE_ROWS, tile), 0)
        mixed_gate = jnp.where(line < 3, -1.0, 0.0)
        for n in range(3):
            mixed_gate = jnp.where(line == 3 + n, q_gate[n : n + 1, :], mixed_gate)
        q = jnp.concatenate(
            [
                jnp.concatenate(pieces, axis=1),
                mixed_gate.astype(BF16),
                jnp.zeros((LANES - size - GATE_ROWS, tile), BF16),
            ],
            axis=0,
        )

        def produce(ref, i, masked=False):
            at = pl.ds(pl.multiple_of(i * block, block), block)
            s = jnp.dot(kbuf[at, :], q, preferred_element_type=F32)
            if masked:
                key = i * block + lax.broadcasted_iota(jnp.int32, (block, tile), 0)
                query = j * tile + lax.broadcasted_iota(jnp.int32, (block, tile), 1)
                s = jnp.where(key <= query, s, -jnp.inf)
            ref[...] = s
            return jnp.max(s, axis=0, keepdims=True)

        def consume(ref, highest, i, state):
            top, total, acc = state
            at = pl.ds(pl.multiple_of(i * block, block), block)
            new_top = jnp.maximum(top, highest)
            p = jnp.exp(ref[...] - new_top)
            scale = jnp.exp(top - new_top)
            total = total * scale + jnp.sum(p, axis=0, keepdims=True)
            acc = acc * scale + jnp.dot(vbuf[:, at], p.astype(BF16), preferred_element_type=F32)
            return new_top, total, acc

        fresh = (
            jnp.full((1, tile), -1e30, F32),
            jnp.zeros((1, tile), F32),
            jnp.zeros((size, tile), F32),
        )
        full = j * tile // block

        def save(state):
            kept_top[k], kept_total[k], kept_acc[k] = state

        if second:
            low = 0
            high_end = jnp.where(near, half_blocks, full)

            @pl.when(jnp.logical_not(near))
            def _():
                high = produce(even, full, True)
                save(consume(even, high, full, fresh))

            high_next = produce(odd, low)
            state = (kept_top[k], kept_total[k], kept_acc[k])
        else:
            low = jnp.where(upper, half_blocks, 0)
            high_end = full
            high = produce(even, full, True)
            high_next = produce(odd, low)
            state = consume(even, high, full, fresh)

        def two(i, carry):
            high, state = carry
            high_next = produce(even, low + 2 * i + 1)
            state = consume(odd, high, low + 2 * i, state)
            high = produce(odd, low + 2 * i + 2)
            state = consume(even, high_next, low + 2 * i + 1, state)
            return high, state

        pairs = (high_end - low) // 2
        high, state = lax.fori_loop(0, pairs, two, (high_next, state))
        state = lax.fori_loop(
            low + 2 * pairs, high_end, lambda i, st: consume(odd, high, i, st), state
        )
        if second:
            emit(k, j, state)
        else:
            pl.when(upper)(lambda: save(state))
            pl.when(jnp.logical_not(upper))(lambda: emit(k, j, state))

    def emit(k, j, state):
        top, total, acc = state
        done = (acc / total).astype(BF16)
        for p in range(per_tile):
            slot = k * per_tile + p
            att_stage[slot] = done[:, p * LANES : (p + 1) * LANES]
        for p in range(per_tile):
            slot = k * per_tile + p
            g = j * per_tile + p
            owner, copy = att_copy(g, slot)
            mine = (owner == me) & (src_tp == tp)

            @pl.when(jnp.logical_not(mine))
            def _():
                copy.start()

            @pl.when(mine)
            def _():
                att_local(g, slot).start()

    def first_pass(k, carry):
        pl.when((tile_of(k) >= half_tiles) == upper)(lambda: attend(k, False))
        return carry

    def second_pass(k, carry):
        pl.when(upper | (tile_of(k) >= half_tiles))(lambda: attend(k, True))
        return carry

    take_half(jnp.where(upper, half, 0))
    lax.fori_loop(0, rounds, first_pass, 0)
    take_half(jnp.where(upper, 0, half))
    lax.fori_loop(0, rounds, second_pass, 0)

    loads[3].wait()

    def att_wait(at, carry):
        h = at // per_chunk
        p = lax.rem(at, per_chunk)
        pltpu.make_async_remote_copy(
            src_ref=att_stage.at[0], dst_ref=att_all.at[h, p],
            send_sem=att_send.at[0], recv_sem=att_recv.at[at],
            device_id=(me, pair + 1 - core), device_id_type=MESH,
        ).wait_recv()
        return carry

    lax.fori_loop(0, heads * per_chunk, att_wait, 0)
    for p in range(per_chunk):
        joined = jnp.concatenate([att_all[h, p] for h in range(heads)], axis=0)
        att_rows[p * LANES : (p + 1) * LANES, :] = joined.T

    def part_copy(step):
        peer = lax.rem(tp + step, n_tp)
        return pltpu.make_async_remote_copy(
            src_ref=part.at[peer], dst_ref=part_in.at[step],
            send_sem=part_send.at[step], recv_sem=part_recv.at[step],
            device_id=(me, peer), device_id_type=MESH,
        )

    model = wo.shape[1]
    out_cols = math.gcd(model, 512)

    def project_rows(step, carry):
        peer = lax.rem(tp + step, n_tp)
        rows = att_rows[pl.ds(pl.multiple_of(peer * own_rows, math.gcd(own_rows, LANES)), own_rows), :]

        def columns(c, carry):
            at = pl.ds(pl.multiple_of(c * out_cols, out_cols), out_cols)
            part[peer, :, at] = jnp.dot(rows, wo[:, at], preferred_element_type=F32).astype(BF16)
            return carry

        lax.fori_loop(0, model // out_cols, columns, 0)
        return carry

    for step in range(1, n_tp):
        project_rows(step, 0)
        part_copy(step).start()
    project_rows(0, 0)
    for step in range(1, n_tp):
        part_copy(step).wait_recv()

    def finish(c, carry):
        at = pl.ds(pl.multiple_of(c * out_cols, out_cols), out_cols)
        mixed = part[tp, :, at].astype(F32)
        for step in range(1, n_tp):
            mixed = mixed + part_in[step, :, at].astype(F32)
        out_ref[:, at] = mixed.astype(BF16)
        return carry

    lax.fori_loop(0, model // out_cols, finish, 0)

    for step in range(1, n_tp):
        part_copy(step).wait_send()

    def sent_slab(at_send, carry):
        h = at_send // copies
        r = lax.rem(at_send, copies)
        chip, target, copy = slab_copy(h, r, me)

        @pl.when(jnp.logical_not((chip == me) & (target == tp)))
        def _():
            copy.wait_send()

        return carry

    lax.fori_loop(0, heads * copies, sent_slab, 0)

    def sent_fwd(k, carry):
        fwd_copy(2 * k + core).wait_send()
        return carry

    lax.fori_loop(0, n_sp // 2, sent_fwd, 0)

    def sent_att(k, carry):
        j = tile_of(k)
        for p in range(per_tile):
            owner, copy = att_copy(j * per_tile + p, k * per_tile + p)

            @pl.when(jnp.logical_not((owner == me) & (src_tp == tp)))
            def _():
                copy.wait_send()

        return carry

    lax.fori_loop(0, rounds, sent_att, 0)


def on_device(n_sp, n_tp, tokens, wq, wk, wv, q_gain, k_gain, gates, wo):
    own_rows, model = tokens.shape
    shard_rows, heads = gates.shape
    width = wq.shape[1]
    size = width // heads
    copies = n_sp // (2 * heads)
    total = n_sp * shard_rows
    tile, block = 256, 1024
    rounds = total // tile // (2 * copies)
    slab_rows = 3 * size + GATE_ROWS
    per_tile = tile // LANES
    per_chunk = shard_rows // LANES
    hbm = pl.BlockSpec(memory_space=pl.ANY)
    vmem = pl.BlockSpec(memory_space=pltpu.VMEM)
    dma = pltpu.SemaphoreType.DMA
    return pl.pallas_call(
        functools.partial(kernel, n_sp, n_tp, heads, size, shard_rows, tile, block),
        out_shape=jax.ShapeDtypeStruct((own_rows, model), BF16),
        in_specs=[hbm, hbm, hbm, hbm, vmem, vmem, vmem, hbm],
        out_specs=vmem,
        scratch_shapes=[
            pltpu.VMEM((n_tp, own_rows, model), BF16),
            pltpu.VMEM(wq.shape, BF16),
            pltpu.VMEM(wk.shape, BF16),
            pltpu.VMEM(wv.shape, BF16),
            pltpu.VMEM(wo.shape, BF16),
            pltpu.VMEM((heads, slab_rows, shard_rows), BF16),
            pltpu.VMEM((n_sp, slab_rows, shard_rows), BF16),
            pltpu.VMEM((total, LANES), BF16),
            pltpu.VMEM((size, total), BF16),
            pltpu.VMEM((rounds * per_tile, size, LANES), BF16),
            pltpu.VMEM((heads, per_chunk, size, LANES), BF16),
            pltpu.VMEM((shard_rows, width), BF16),
            pltpu.VMEM((n_tp, own_rows, model), BF16),
            pltpu.VMEM((n_tp, own_rows, model), BF16),
            pltpu.VMEM((block, tile), F32),
            pltpu.VMEM((block, tile), F32),
            pltpu.VMEM((rounds, 1, tile), F32),
            pltpu.VMEM((rounds, 1, tile), F32),
            pltpu.VMEM((rounds, size, tile), F32),
            dma((5,)),
            dma((n_tp,)),
            dma((n_tp,)),
            dma((heads * copies,)),
            dma((n_sp,)),
            dma((n_sp,)),
            dma((rounds * per_tile,)),
            dma((heads * per_chunk,)),
            dma((n_tp,)),
            dma((n_tp,)),
        ],
        compiler_params=pltpu.CompilerParams(
            has_side_effects=True, collective_id=0, vmem_limit_bytes=60 * 1024 * 1024
        ),
    )(
        tokens, wq, wk, wv,
        q_gain.reshape(1, size), k_gain.reshape(1, size),
        gates.T, wo,
    )


def solution(mesh):
    placed = (
        P(("sp", "tp"), None),
        P(None, "tp"),
        P(None, "tp"),
        P(None, "tp"),
        P(),
        P(),
        P("sp", "tp"),
        P("tp", None),
    )
    return jax.shard_map(
        functools.partial(on_device, mesh.shape["sp"], mesh.shape["tp"]),
        mesh=mesh, in_specs=placed, out_specs=P(("sp", "tp"), None), check_vma=False,
    )
```
